32 devices in a mesh: sp: 8 (over z, y), tp: 4 (over x, core).
Axes of the slice: x: 2, y: 2, z: 4, core: 2. Of those that a mesh axis runs over, the one named last changes fastest.
Arguments:
- residual: bfloat16 [2048, 2048], P('sp'), may hold values from -6 to 6
- queries: bfloat16 [2048, 8, 128], P('sp', 'tp'), may hold values from -100 to 100
- keys: bfloat16 [2048, 8, 128], P('sp', 'tp'), may hold values from -60 to 60
- values: bfloat16 [2048, 8, 128], P('sp', 'tp'), may hold values from -6 to 6
- documents: int32 [2048], P('sp'), may hold values from 0 to 7, never falling along the last dimension, each value on 1 to 1024 neighbouring positions
- lambdas: float32 [8], P('tp'), may hold values from 0.3 to 0.8
- head_gain: float32 [8, 128], P('tp'), may hold values from 0.1 to 1.9
- out_weight: bfloat16 [1024, 2048], replicated, may hold values from -0.1875 to 0.1875
- mix_gain: float32 [2048], replicated, may hold values from 0.1 to 1.9
- pre_gain: float32 [2048], replicated, may hold values from 0.1 to 1.9
- gate_weight: bfloat16 [2048, 3072], P('sp', 'tp'), may hold values from -0.125 to 0.125
- value_weight: bfloat16 [2048, 3072], P('sp', 'tp'), may hold values from -0.125 to 0.125
- gate_taps: float32 [3, 3072], P(None, 'tp'), may hold values from -3 to 3
- value_taps: float32 [3, 3072], P(None, 'tp'), may hold values from -3 to 3
- down_weight: bfloat16 [2048, 3072], P('sp', 'tp'), may hold values from -0.109375 to 0.109375
- mlp_gain: float32 [2048], replicated, may hold values from 0.1 to 1.9
Outputs:
- out: bfloat16 [2048, 2048], P('sp')
The draws below stay inside these ranges and needn't reach their ends.
All inputs are finite; a program needn't handle non-finite values.
Results may differ from the reference program's by a relative error of at most 0.015.
Values may be sent and summed in bfloat16 or wider, within the bound.
A program may use at most 128 MiB of HBM per device.

```python
import math
import jax
import jax.numpy as jnp
import numpy as np
from jax import lax

D = 2048
HEADS = 8
QK = 64
HEAD_DIM = 128
FF = 3072
TAPS = 3
DOCS = 8
TOKENS = 2048
N_TP = 4


def draw_queries(key, part):
    random_part = jnp.clip(1.3 * jax.random.normal(jax.random.fold_in(key, 1), (TOKENS, HEADS, 2, QK), jnp.float32), -6.5, 6.5)
    return random_part.reshape(TOKENS, HEADS, 2 * QK).astype(jnp.bfloat16)


def draw_keys(key, part):
    random_part = jnp.clip(1.3 * jax.random.normal(jax.random.fold_in(key, 2), (TOKENS, HEADS, 2, QK), jnp.float32), -6.5, 6.5)
    return random_part.reshape(TOKENS, HEADS, 2 * QK).astype(jnp.bfloat16)


def block_scale(stream_key, shape, pieces, least, top_value):
    def one(position, shards_of):
        heights = jax.random.uniform(jax.random.fold_in(jax.random.fold_in(stream_key, 6), position), (shards_of,), jnp.float32, least / len(pieces), top_value / len(pieces))
        return jnp.repeat(jnp.exp(heights), shape[position] // shards_of).reshape((-1,) + (1,) * (len(shape) - position - 1))

    level = one(*pieces[0])
    for cut in pieces[1:]:
        level = level * one(*cut)
    return level


def length_profile(count, total, limit, lean):
    portions = [(1 << 20) // math.isqrt(standing ** lean) + 1 for standing in range(2, count + 1)]
    rest, given = total - limit - (count - 1), [1] * (count - 1)
    while rest > 0:
        movable = [i for i in range(count - 1) if given[i] < limit]
        pool, left = sum([portions[i] for i in movable]), rest
        for i in movable:
            more = min(limit - given[i], max(1, left * portions[i] // pool), rest)
            given[i] = given[i] + more
            rest = rest - more
    return np.array([limit] + given)


def ragged(rng, number_of, total, most, skew):
    if number_of == 2:
        one = jax.random.randint(rng, (), max(1, total - most), min(most, total - 1) + 1)
        return jnp.stack([one, total - one])
    sizes = jnp.asarray(length_profile(number_of, total, most, skew), jnp.int32)
    pairs = (number_of - 1) // 2
    giver, receiver = sizes[1:1 + 2 * pairs:2], sizes[2:2 + 2 * pairs:2]
    room = jnp.minimum(giver - 1, most - receiver)
    shifted = jax.random.randint(jax.random.fold_in(rng, 1), (pairs,), 0, 1 << 20) % (room + 1)
    sizes = sizes.at[1:1 + 2 * pairs:2].set(giver - shifted).at[2:2 + 2 * pairs:2].set(receiver + shifted)
    return sizes[jax.random.permutation(jax.random.fold_in(rng, 2), number_of)]


def normal_values(key, extent, deviation, most, cuts=(), kind=jnp.bfloat16):
    values = jax.random.normal(key, extent, jnp.float32) * deviation
    if len(cuts) > 0:
        values = block_scale(key, extent, cuts, -0.22, 0.18) * values
    return jnp.clip(values, min=-most, max=most).astype(kind)


def setup_inputs(seed: int = 0) -> dict:
    splits = jax.random.split(jax.random.key(seed), 17)
    residual = normal_values(splits[0], (TOKENS, D), 1.0, 6.0, ((0, 8),))
    queries = draw_queries(jax.random.fold_in(splits[16], 71), 0)
    keys = draw_keys(jax.random.fold_in(splits[16], 71), 0)
    values = normal_values(splits[3], (TOKENS, HEADS, HEAD_DIM), 1.0, 6.0, ((0, 8), (1, 4)))
    documents = jnp.searchsorted(jnp.cumsum(ragged(splits[4], DOCS, TOKENS, TOKENS // 2, 0)), jnp.arange(TOKENS), side="right").astype(jnp.int32)
    lambdas = jnp.clip(0.3 + 0.5 * jax.random.uniform(splits[5], (HEADS,), jnp.float32) ** block_scale(splits[5], (HEADS,), ((0, 4),), -0.2, 0.2), 0.3, 0.8)
    head_gain = jnp.clip(1.0 + 0.18 * jax.random.normal(splits[6], (HEADS, HEAD_DIM), jnp.float32), 0.1, 1.9)
    out_weight = normal_values(splits[7], (HEADS * HEAD_DIM, D), (HEADS * HEAD_DIM) ** -0.5, 0.1875)
    mix_gain = jnp.clip(1.0 + 0.18 * jax.random.normal(splits[8], (D,), jnp.float32), 0.1, 1.9)
    pre_gain = jnp.clip(1.0 + 0.18 * jax.random.normal(splits[9], (D,), jnp.float32), 0.1, 1.9)
    gate_weight = normal_values(splits[10], (D, FF), D ** -0.5, 0.125, ((0, 8), (1, 4)))
    value_weight = normal_values(splits[11], (D, FF), D ** -0.5, 0.125, ((0, 8), (1, 4)))
    gate_taps = normal_values(splits[12], (TAPS, FF), 0.577, 3.0, ((1, 4),), jnp.float32)
    value_taps = normal_values(splits[13], (TAPS, FF), 0.577, 3.0, ((1, 4),), jnp.float32)
    down_weight = normal_values(splits[14], (D, FF), FF ** -0.5, 0.109375, ((0, 8), (1, 4)))
    mlp_gain = jnp.clip(1.0 + 0.18 * jax.random.normal(splits[15], (D,), jnp.float32), 0.1, 1.9)
    return dict(residual=residual, queries=queries, keys=keys, values=values, documents=documents, lambdas=lambdas, head_gain=head_gain, out_weight=out_weight, mix_gain=mix_gain, pre_gain=pre_gain, gate_weight=gate_weight, value_weight=value_weight, gate_taps=gate_taps, value_taps=value_taps, down_weight=down_weight, mlp_gain=mlp_gain)


epsilon = 1e-06

def rms_scale(values_in, gain):
    return values_in * lax.rsqrt(lax.optimization_barrier(jnp.mean(values_in * values_in, axis=-1, keepdims=True)) + epsilon) * gain

def reference(residual, queries, keys, values, documents, lambdas, head_gain, out_weight, mix_gain, pre_gain, gate_weight, value_weight, gate_taps, value_taps, down_weight, mlp_gain):
    query_block = math.gcd(TOKENS, 256)
    queries_wide = queries.astype(jnp.float32)
    keys_wide = keys.astype(jnp.float32)
    values_wide = values.astype(jnp.float32)
    positions = jnp.arange(TOKENS, dtype=jnp.int32)
    score_scale = QK ** (-0.5)

    def one_block(number):
        first_row = number * query_block
        query_rows = lax.dynamic_slice_in_dim(queries_wide, first_row, query_block, 0)
        query_pos = first_row + jnp.arange(query_block, dtype=jnp.int32)
        query_docs = lax.dynamic_slice_in_dim(documents, first_row, query_block, 0)
        allowed = (positions[None, :] <= query_pos[:, None]) & (documents[None, :] == query_docs[:, None])
        results = []
        for map_index in range(2):
            query_part = query_rows[:, :, map_index * QK:(map_index + 1) * QK]
            key_part = keys_wide[:, :, map_index * QK:(map_index + 1) * QK]
            scores = jnp.einsum('qhd,khd->hqk', query_part, key_part) * score_scale
            scores = jnp.where(allowed[None], scores, -jnp.inf)
            probs = jax.nn.softmax(scores, axis=-1).astype(jnp.bfloat16)
            probs = lax.optimization_barrier(probs).astype(jnp.float32)
            results.append(jnp.einsum('hqk,khe->qhe', probs, values_wide))
        return results[0] - lambdas[None, :, None] * results[1]
    heads = lax.map(one_block, jnp.arange(TOKENS // query_block, dtype=jnp.int32))
    heads = heads.reshape(TOKENS, HEADS, HEAD_DIM)
    normed = rms_scale(heads, head_gain[None]).astype(jnp.bfloat16).reshape(TOKENS, HEADS * HEAD_DIM)
    mixed = jnp.dot(normed, out_weight, preferred_element_type=jnp.float32)
    stream = residual.astype(jnp.float32) + rms_scale(mixed, mix_gain)
    normal_input = rms_scale(stream, pre_gain).astype(jnp.bfloat16)
    gate_pre = jnp.dot(normal_input, gate_weight, preferred_element_type=jnp.float32).astype(jnp.bfloat16)
    value_pre = jnp.dot(normal_input, value_weight, preferred_element_type=jnp.float32).astype(jnp.bfloat16)
    reach = TAPS - 1
    earlier_docs = jnp.concatenate([jnp.full((reach,), -1, dtype=jnp.int32), documents.astype(jnp.int32)])

    def convolve(pre_values, tap_rows):
        extended = jnp.pad(lax.optimization_barrier(pre_values).astype(jnp.float32), ((reach, 0), (0, 0)))
        summed = jnp.zeros((TOKENS, FF), jnp.float32)
        for shift_by in range(TAPS):
            same_doc = (earlier_docs[shift_by:shift_by + TOKENS] == documents)[:, None]
            summed = summed + jnp.where(same_doc, tap_rows[shift_by][None, :] * extended[shift_by:shift_by + TOKENS], 0.0)
        return summed
    hidden = (jax.nn.gelu(convolve(gate_pre, gate_taps), approximate=True) * convolve(value_pre, value_taps)).astype(jnp.bfloat16)
    group = FF // N_TP
    lifted = jnp.zeros((TOKENS, D), jnp.float32)
    for member in range(N_TP):
        term = lax.dot_general(hidden[:, member * group:(member + 1) * group], down_weight[:, member * group:(member + 1) * group], (((1,), (1,)), ((), ())), preferred_element_type=jnp.float32).astype(jnp.bfloat16)
        lifted = lifted + lax.optimization_barrier(term).astype(jnp.float32)
    return (stream + rms_scale(lifted, mlp_gain)).astype(jnp.bfloat16)
```

```python
import functools

import jax
import jax.numpy as jnp
from jax import lax
from jax.experimental import pallas as pl
from jax.experimental.pallas import tpu as pltpu
from jax.sharding import PartitionSpec as P

epsilon = 1e-06
masked_score = -1e30
EXTRA = 32
KV, GATE, VALUE, DOWN = range(4)


def kernel(
    n,
    ntp,
    lam_ref,
    kv_hbm,
    g_hbm,
    v_hbm,
    d_hbm,
    ow_hbm,
    res_hbm,
    q_ref,
    dcol_ref,
    hg_ref,
    mixg_ref,
    preg_ref,
    gt_ref,
    vt_ref,
    mlpg_ref,
    out_ref,
    kvb,
    gb,
    vb,
    db,
    owb,
    resb,
    nrm,
    stream,
    xn,
    gacc,
    vacc,
    gext,
    vext,
    halo_out,
    halo_in,
    hidden,
    part,
    rsb,
    mrow,
    lrow,
    att,
    local_sem,
    ring_send,
    ring_recv,
    nrm_send,
    nrm_recv,
    halo_send,
    halo_recv,
    rs_send,
    rs_recv,
    ag_send,
    ag_recv,
):
    s = lax.axis_index("sp")
    t = lax.axis_index("tp")
    half = n // 2
    tok = resb.shape[0]
    width = resb.shape[1]
    rows = g_hbm.shape[0]
    ff = g_hbm.shape[1]
    heads = hg_ref.shape[0]
    hd = hg_ref.shape[1]
    hw = heads * hd
    share = tok // ntp
    pos = jnp.where(s % 2 == 0, s // 2, n - 1 - s // 2)

    def at(p):
        p = (p + n) % n
        return jnp.where(p < half, 2 * p, 2 * n - 1 - 2 * p)

    neighbour = (at(pos + 1), at(pos - 1))

    def place(kind, owner, piece):
        if kind == KV:
            size = kvb.shape[1]
            if piece is None:
                return kvb.at[owner]
            return kvb.at[owner, pl.ds(piece * (size // 2), size // 2)]
        ref = (None, gb, vb, db)[kind]
        if piece is None:
            return ref.at[pl.ds(pl.multiple_of(owner * rows, rows), rows)]
        return ref.at[pl.ds(pl.multiple_of(owner * rows + piece * (rows // 2), rows // 2), rows // 2)]

    def hop(kind, way, step, owner):
        ref = place(kind, owner, way if step == half else None)
        return pltpu.make_async_remote_copy(
            src_ref=ref,
            dst_ref=ref,
            send_sem=ring_send.at[kind, way, step - 1],
            recv_sem=ring_recv.at[kind, way, step - 1],
            device_id={"sp": neighbour[way]},
            device_id_type=pl.DeviceIdType.MESH,
        )

    def came(way, step):
        return at(pos - step) if way == 0 else at(pos + step)

    def send(kind, way, step):
        hop(kind, way, step, came(way, step - 1)).start()

    def arrive(kind, way, step):
        hop(kind, way, step, came(way, step)).wait_recv()

    local = [
        pltpu.make_async_copy(src, dst, local_sem.at[i])
        for i, (src, dst) in enumerate(
            (
                (kv_hbm, kvb.at[s]),
                (g_hbm, place(GATE, s, None)),
                (v_hbm, place(VALUE, s, None)),
                (d_hbm, place(DOWN, s, None)),
                (ow_hbm, owb),
                (res_hbm, resb),
            )
        )
    ]
    for copy in local:
        copy.start()
    local[0].wait()
    for way in range(2):
        send(KV, way, 1)
    for step in range(1, half):
        for way in range(2):
            arrive(KV, way, step)
            send(KV, way, step + 1)
    for i in (1, 2, 3):
        local[i].wait()
    for kind in (GATE, VALUE, DOWN):
        for way in range(2):
            send(kind, way, 1)
    for way in range(2):
        arrive(KV, way, half)

    mrow[...] = jnp.full(mrow.shape, masked_score, jnp.float32)
    lrow[...] = jnp.zeros(lrow.shape, jnp.float32)
    att[...] = jnp.zeros(att.shape, jnp.float32)
    doc_query = dcol_ref[:, 0:1]
    lane = lax.broadcasted_iota(jnp.int32, (tok, hd), 1)
    delta = lax.broadcasted_iota(jnp.int32, (tok, tok), 0) - lax.broadcasted_iota(
        jnp.int32, (tok, tok), 1
    )

    @pl.loop(0, jnp.minimum(s, half) + 1)
    def _(back):
        o = s - back
        doc_key = kvb[o, pl.ds(tok, 16), pl.ds(0, tok)].astype(jnp.float32)[0:1]
        allowed = (delta + back * tok >= 0) & (doc_key == doc_query)
        for h in range(heads):
            k = kvb[o, pl.ds(0, tok), pl.ds(h * hd, hd)]
            val = kvb[o, pl.ds(0, tok), pl.ds(hw + h * hd, hd)]
            qh = q_ref[:, h * hd : (h + 1) * hd]
            for m in range(2):
                keep = lane < hd // 2 if m == 0 else lane >= hd // 2
                qm = jnp.where(keep, qh, jnp.zeros_like(qh))
                scores = lax.dot_general(
                    qm, k, (((1,), (1,)), ((), ())), preferred_element_type=jnp.float32
                )
                scores = jnp.where(allowed, scores, masked_score)
                idx = h * 2 + m
                old = mrow[idx, :, 0:1]
                new = jnp.maximum(old, jnp.max(scores, axis=1, keepdims=True))
                probs = jnp.where(allowed, jnp.exp(scores - new), 0.0)
                factor = jnp.exp(old - new)
                total = lrow[idx, :, 0:1] * factor + jnp.sum(probs, axis=1, keepdims=True)
                att[idx] = att[idx] * factor + jnp.dot(
                    probs.astype(jnp.bfloat16), val, preferred_element_type=jnp.float32
                )
                mrow[idx] = jnp.broadcast_to(new, (tok, hd))
                lrow[idx] = jnp.broadcast_to(total, (tok, hd))

    for h in range(heads):
        head = att[2 * h] / lrow[2 * h] - lam_ref[h] * (att[2 * h + 1] / lrow[2 * h + 1])
        scale = lax.rsqrt(jnp.mean(head * head, axis=1, keepdims=True) + epsilon)
        nrm[t, :, pl.ds(h * hd, hd)] = (head * scale * hg_ref[h : h + 1, :]).astype(jnp.bfloat16)

    def peer_copy(src, dst, send_sem, recv_sem, i):
        return pltpu.make_async_remote_copy(
            src_ref=src,
            dst_ref=dst,
            send_sem=send_sem,
            recv_sem=recv_sem,
            device_id={"tp": (t + i) % ntp},
            device_id_type=pl.DeviceIdType.MESH,
        )

    def nrm_copy(i, slot):
        return peer_copy(nrm.at[slot], nrm.at[slot], nrm_send.at[i], nrm_recv.at[i], i)

    for i in range(1, ntp):
        nrm_copy(i, t).start()
    local[4].wait()
    local[5].wait()
    for i in range(1, ntp):
        nrm_copy(i, (t - i + ntp) % ntp).wait_recv()

    tile = 256

    @pl.loop(0, width // tile)
    def _(c):
        cols = pl.ds(pl.multiple_of(c * tile, tile), tile)
        acc = jnp.zeros((tok, tile), jnp.float32)
        for j in range(ntp):
            acc = acc + jnp.dot(
                nrm[j], owb[pl.ds(j * hw, hw), cols], preferred_element_type=jnp.float32
            )
        stream[:, cols] = acc

    def rms(x, gain):
        return x * lax.rsqrt(jnp.mean(x * x, axis=1, keepdims=True) + epsilon) * gain

    chunk = 16

    @pl.loop(0, tok // chunk)
    def _(c):
        part_rows = pl.ds(pl.multiple_of(c * chunk, chunk), chunk)
        st = resb[part_rows].astype(jnp.float32) + rms(stream[part_rows], mixg_ref[...])
        stream[part_rows] = st
        xn[part_rows] = rms(st, preg_ref[...]).astype(jnp.bfloat16)

    fine = rows % 128 == 0

    def add_block(kind, owner, first):
        acc, w = (gacc, gb) if kind == GATE else (vacc, vb)
        at_rows = pl.ds(pl.multiple_of(owner * rows, rows), rows)
        got = jnp.dot(xn[:, at_rows], w[at_rows, :], preferred_element_type=jnp.float32)
        if first:
            acc[...] = got
        else:
            acc[...] += got

    if fine:
        for kind in (GATE, VALUE):
            add_block(kind, s, True)
    for step in range(1, half + 1):
        for kind in (GATE, VALUE):
            for way in range(2):
                arrive(kind, way, step)
                if step < half:
                    send(kind, way, step + 1)
            if step == half and kind == VALUE:
                for way in range(2):
                    arrive(DOWN, way, 1)
                    send(DOWN, way, 2)
            if fine:
                add_block(kind, came(0, step), False)
                if step < half:
                    add_block(kind, came(1, step), False)
    if not fine:
        gacc[...] = jnp.dot(xn[...], gb[...], preferred_element_type=jnp.float32)
        vacc[...] = jnp.dot(xn[...], vb[...], preferred_element_type=jnp.float32)

    for i, (acc, ext) in enumerate(((gacc, gext), (vacc, vext))):
        ext[pl.ds(8, tok), :] = acc[...].astype(jnp.bfloat16).astype(jnp.float32)
        halo_out[i] = acc[pl.ds(tok - 16, 16), :].astype(jnp.bfloat16)
        ext[pl.ds(0, 8), :] = jnp.zeros((8, ff), jnp.float32)

    def halo(target):
        return pltpu.make_async_remote_copy(
            src_ref=halo_out,
            dst_ref=halo_in,
            send_sem=halo_send,
            recv_sem=halo_recv,
            device_id={"sp": target},
            device_id_type=pl.DeviceIdType.MESH,
        )

    @pl.when(s < n - 1)
    def _():
        halo(s + 1).start()

    @pl.when(s > 0)
    def _():
        halo(s - 1).wait_recv()
        for i, ext in enumerate((gext, vext)):
            ext[pl.ds(0, 8), :] = halo_in[i].astype(jnp.float32)[8:16]

    before = jnp.maximum(s - 1, 0)
    prev_docs = kvb[before, pl.ds(tok, 16), pl.ds(0, tok)].astype(jnp.float32)[0:1]
    lane_row = lax.broadcasted_iota(jnp.int32, (1, tok), 1)
    last1 = jnp.sum(jnp.where(lane_row == tok - 1, prev_docs, 0.0), axis=1, keepdims=True)
    last2 = jnp.sum(jnp.where(lane_row == tok - 2, prev_docs, 0.0), axis=1, keepdims=True)
    has_prev = s > 0
    last1 = jnp.where(has_prev, last1, -1.0)
    last2 = jnp.where(has_prev, last2, -1.0)
    rowid = lax.broadcasted_iota(jnp.int32, (tok, 1), 0)
    doc1 = jnp.where(rowid == 0, last1, dcol_ref[:, 1:2])
    doc2 = jnp.where(rowid == 0, last2, jnp.where(rowid == 1, last1, dcol_ref[:, 2:3]))
    same1 = doc1 == doc_query
    same2 = doc2 == doc_query

    @pl.loop(0, ff // 128)
    def _(c):
        cols = pl.ds(pl.multiple_of(c * 128, 128), 128)

        def conv(ext, taps):
            w = taps[:, cols]
            total = jnp.where(same2, w[0:1] * ext[pl.ds(6, tok), cols], 0.0)
            total = total + jnp.where(same1, w[1:2] * ext[pl.ds(7, tok), cols], 0.0)
            return total + w[2:3] * ext[pl.ds(8, tok), cols]

        hidden[:, cols] = (
            jax.nn.gelu(conv(gext, gt_ref), approximate=True) * conv(vext, vt_ref)
        ).astype(jnp.bfloat16)

    def rs_copy(i, b, cols):
        peer = (t + i) % ntp
        return peer_copy(
            part.at[pl.ds(pl.multiple_of(peer * share, share), share), cols],
            rsb.at[i - 1, :, cols],
            rs_send.at[b, i],
            rs_recv.at[b, i],
            i,
        )

    def block_cols(owner):
        return pl.ds(pl.multiple_of(owner * rows, rows), rows)

    def down_block(owner, b):
        cols = block_cols(owner)
        part[:, cols] = lax.dot_general(
            hidden[...], db[cols, :], (((1,), (1,)), ((), ())), preferred_element_type=jnp.float32
        ).astype(jnp.bfloat16)
        for i in range(1, ntp):
            rs_copy(i, b, cols).start()

    order = [s]
    if fine:
        down_block(s, 0)
    for step in range(1, half + 1):
        for way in range(2):
            if step > 1:
                arrive(DOWN, way, step)
                if step < half:
                    send(DOWN, way, step + 1)
        for way in range(2 if step < half else 1):
            if fine:
                down_block(came(way, step), len(order))
                order.append(came(way, step))
    if fine:
        pieces = [(b, block_cols(o)) for b, o in enumerate(order)]
    else:

        @pl.loop(0, width // tile)
        def _(c):
            cols = pl.ds(pl.multiple_of(c * tile, tile), tile)
            part[:, cols] = lax.dot_general(
                hidden[...],
                db[cols, :],
                (((1,), (1,)), ((), ())),
                preferred_element_type=jnp.float32,
            ).astype(jnp.bfloat16)

        pieces = [(0, pl.ds(0, width))]
        for i in range(1, ntp):
            rs_copy(i, 0, pieces[0][1]).start()
    for b, cols in pieces:
        for i in range(1, ntp):
            rs_copy(i, b, cols).wait_recv()

    mine = pl.multiple_of(t * share, share)

    @pl.loop(0, share // chunk)
    def _(c):
        at_rows = pl.ds(pl.multiple_of(mine + c * chunk, chunk), chunk)
        in_rows = pl.ds(pl.multiple_of(c * chunk, chunk), chunk)
        lifted = part[at_rows].astype(jnp.float32)
        for i in range(1, ntp):
            lifted = lifted + rsb[i - 1, in_rows].astype(jnp.float32)
        out_ref[at_rows] = (stream[at_rows] + rms(lifted, mlpg_ref[...])).astype(jnp.bfloat16)

    def ag_copy(i, owner):
        ref = out_ref.at[pl.ds(pl.multiple_of(owner * share, share), share)]
        return peer_copy(ref, ref, ag_send.at[i], ag_recv.at[i], i)

    for i in range(1, ntp):
        ag_copy(i, t).start()
    for i in range(1, ntp):
        ag_copy(i, (t - i + ntp) % ntp).wait_recv()

    for kind in (KV, GATE, VALUE, DOWN):
        for way in range(2):
            for step in range(1, half + 1):
                hop(kind, way, step, came(way, step - 1)).wait_send()
    for i in range(1, ntp):
        nrm_copy(i, t).wait_send()
        for b, cols in pieces:
            rs_copy(i, b, cols).wait_send()
        ag_copy(i, t).wait_send()

    @pl.when(s < n - 1)
    def _():
        halo(s + 1).wait_send()


def per_device(
    n,
    ntp,
    residual,
    queries,
    keys,
    values,
    documents,
    lambdas,
    head_gain,
    out_weight,
    mix_gain,
    pre_gain,
    gate_weight,
    value_weight,
    gate_taps,
    value_taps,
    down_weight,
    mlp_gain,
):
    tok, width = residual.shape
    heads, hd = head_gain.shape
    hw = heads * hd
    rows, ff = gate_weight.shape
    half = n // 2
    share = tok // ntp
    docs = documents.astype(jnp.float32)
    packed = jnp.concatenate([keys.reshape(tok, hw), values.reshape(tok, hw)], axis=1)
    doc_rows = jnp.broadcast_to(
        jnp.pad(docs, (0, 2 * hw - tok)).astype(jnp.bfloat16)[None, :], (EXTRA, 2 * hw)
    )
    kv = jnp.concatenate([packed, doc_rows], axis=0)
    back = [jnp.concatenate([jnp.full((j,), -1.0, jnp.float32), docs[: tok - j]]) for j in (1, 2)]
    dcol = jnp.pad(jnp.stack([docs] + back, axis=1), ((0, 0), (0, 125)))
    score_scale = (hd // 2) ** (-0.5)
    q = (queries.astype(jnp.float32) * score_scale).astype(jnp.bfloat16).reshape(tok, hw)
    bf, f32 = jnp.bfloat16, jnp.float32
    vm = pl.BlockSpec(memory_space=pltpu.VMEM)
    hbm = pl.BlockSpec(memory_space=pl.ANY)
    smem = pl.BlockSpec(memory_space=pltpu.SMEM)
    dma = pltpu.SemaphoreType.DMA
    return pl.pallas_call(
        functools.partial(kernel, n, ntp),
        out_shape=jax.ShapeDtypeStruct((tok, width), bf),
        in_specs=[smem] + [hbm] * 6 + [vm] * 8,
        out_specs=vm,
        scratch_shapes=[
            pltpu.VMEM((n, tok + EXTRA, 2 * hw), bf),
            pltpu.VMEM((n * rows, ff), bf),
            pltpu.VMEM((n * rows, ff), bf),
            pltpu.VMEM((n * rows, ff), bf),
            pltpu.VMEM(out_weight.shape, bf),
            pltpu.VMEM((tok, width), bf),
            pltpu.VMEM((ntp, tok, hw), bf),
            pltpu.VMEM((tok, width), f32),
            pltpu.VMEM((tok, width), bf),
            pltpu.VMEM((tok, ff), f32),
            pltpu.VMEM((tok, ff), f32),
            pltpu.VMEM((tok + 8, ff), f32),
            pltpu.VMEM((tok + 8, ff), f32),
            pltpu.VMEM((2, 16, ff), bf),
            pltpu.VMEM((2, 16, ff), bf),
            pltpu.VMEM((tok, ff), bf),
            pltpu.VMEM((tok, width), bf),
            pltpu.VMEM((ntp - 1, share, width), bf),
            pltpu.VMEM((2 * heads, tok, hd), f32),
            pltpu.VMEM((2 * heads, tok, hd), f32),
            pltpu.VMEM((2 * heads, tok, hd), f32),
            dma((6,)),
            dma((4, 2, half)),
            dma((4, 2, half)),
            dma((ntp,)),
            dma((ntp,)),
            dma,
            dma,
            dma((n, ntp)),
            dma((n, ntp)),
            dma((ntp,)),
            dma((ntp,)),
        ],
        compiler_params=pltpu.CompilerParams(
            has_side_effects=True, vmem_limit_bytes=60 * 1024 * 1024
        ),
    )(
        lambdas,
        kv,
        gate_weight,
        value_weight,
        down_weight,
        out_weight,
        residual,
        q,
        dcol,
        head_gain,
        mix_gain[None],
        pre_gain[None],
        gate_taps,
        value_taps,
        mlp_gain[None],
    )


def solution(mesh):
    placed = (
        P("sp", None),
        P("sp", "tp", None),
        P("sp", "tp", None),
        P("sp", "tp", None),
        P("sp"),
        P("tp"),
        P("tp", None),
        P(),
        P(),
        P(),
        P("sp", "tp"),
        P("sp", "tp"),
        P(None, "tp"),
        P(None, "tp"),
        P("sp", "tp"),
        P(),
    )
    body = functools.partial(per_device, mesh.shape["sp"], mesh.shape["tp"])
    return jax.shard_map(
        body, mesh=mesh, in_specs=placed, out_specs=P("sp", None), check_vma=False
    )
```

```python
import functools

import jax
import jax.numpy as jnp
from jax import lax
from jax.experimental import pallas as pl
from jax.experimental.pallas import tpu as pltpu
from jax.sharding import PartitionSpec as P

epsilon = 1e-06
masked_score = -1e30
EXTRA = 16
GATE, VALUE, DOWN = range(3)


def kernel(
    n,
    ntp,
    lam_ref,
    kv_hbm,
    g_hbm,
    v_hbm,
    d_hbm,
    ow_hbm,
    res_hbm,
    q_ref,
    dcol_ref,
    hg_ref,
    mixg_ref,
    preg_ref,
    gt_ref,
    vt_ref,
    mlpg_ref,
    out_ref,
    kvb,
    gb,
    vb,
    db,
    owb,
    resb,
    nrm,
    stream,
    xn,
    gacc,
    vacc,
    gext,
    vext,
    halo_out,
    halo_in,
    hidden,
    part,
    rsb,
    mrow,
    lrow,
    att,
    local_sem,
    ring_send,
    ring_recv,
    up_send,
    up_recv,
    rung_send,
    rung_recv,
    nrm_send,
    nrm_recv,
    halo_send,
    halo_recv,
    rs_send,
    rs_recv,
    ag_send,
    ag_recv,
):
    s = lax.axis_index("sp")
    t = lax.axis_index("tp")
    half = n // 2
    tok = resb.shape[0]
    width = resb.shape[1]
    rows = g_hbm.shape[0]
    ff = g_hbm.shape[1]
    heads = hg_ref.shape[0]
    hd = hg_ref.shape[1]
    hw = heads * hd
    share = tok // ntp
    pos = jnp.where(s % 2 == 0, s // 2, n - 1 - s // 2)

    def at(p):
        p = (p + n) % n
        return jnp.where(p < half, 2 * p, 2 * n - 1 - 2 * p)

    neighbour = (at(pos + 1), at(pos - 1))

    def place(kind, owner, piece):
        ref = (gb, vb, db)[kind]
        if piece is None:
            return ref.at[pl.ds(pl.multiple_of(owner * rows, rows), rows)]
        return ref.at[pl.ds(pl.multiple_of(owner * rows + piece * (rows // 2), rows // 2), rows // 2)]

    def hop(kind, way, step, owner):
        ref = place(kind, owner, way if step == half else None)
        return pltpu.make_async_remote_copy(
            src_ref=ref,
            dst_ref=ref,
            send_sem=ring_send.at[kind, way, step - 1],
            recv_sem=ring_recv.at[kind, way, step - 1],
            device_id={"sp": neighbour[way]},
            device_id_type=pl.DeviceIdType.MESH,
        )

    def came(way, step):
        return at(pos - step) if way == 0 else at(pos + step)

    def send(kind, way, step):
        hop(kind, way, step, came(way, step - 1)).start()

    def arrive(kind, way, step):
        hop(kind, way, step, came(way, step)).wait_recv()

    local = [
        pltpu.make_async_copy(src, dst, local_sem.at[i])
        for i, (src, dst) in enumerate(
            (
                (kv_hbm, kvb.at[s]),
                (g_hbm, place(GATE, s, None)),
                (v_hbm, place(VALUE, s, None)),
                (d_hbm, place(DOWN, s, None)),
                (ow_hbm, owb),
                (res_hbm, resb),
            )
        )
    ]
    for copy in local:
        copy.start()
    mrow[...] = jnp.full(mrow.shape, masked_score, jnp.float32)
    lrow[...] = jnp.zeros(lrow.shape, jnp.float32)
    att[...] = jnp.zeros(att.shape, jnp.float32)
    doc_query = dcol_ref[:, 0:1]
    lane = lax.broadcasted_iota(jnp.int32, (tok, hd), 1)
    delta = lax.broadcasted_iota(jnp.int32, (tok, tok), 0) - lax.broadcasted_iota(
        jnp.int32, (tok, tok), 1
    )

    def attend(back):
        o = s - back
        doc_key = kvb[o, pl.ds(tok, 16), pl.ds(0, tok)].astype(jnp.float32)[0:1]
        allowed = (delta + back * tok >= 0) & (doc_key == doc_query)
        for h in range(heads):
            k = kvb[o, pl.ds(0, tok), pl.ds(h * hd, hd)]
            val = kvb[o, pl.ds(0, tok), pl.ds(hw + h * hd, hd)]
            qh = q_ref[:, h * hd : (h + 1) * hd]
            for m in range(2):
                keep = lane < hd // 2 if m == 0 else lane >= hd // 2
                qm = jnp.where(keep, qh, jnp.zeros_like(qh))
                scores = lax.dot_general(
                    qm, k, (((1,), (1,)), ((), ())), preferred_element_type=jnp.float32
                )
                scores = jnp.where(allowed, scores, masked_score)
                idx = h * 2 + m
                old = mrow[idx, :, 0:1]
                new = jnp.maximum(old, jnp.max(scores, axis=1, keepdims=True))
                probs = jnp.exp(scores - new)
                factor = jnp.exp(old - new)
                total = lrow[idx, :, 0:1] * factor + jnp.sum(probs, axis=1, keepdims=True)
                att[idx] = att[idx] * factor + jnp.dot(
                    probs.astype(jnp.bfloat16), val, preferred_element_type=jnp.float32
                )
                mrow[idx] = jnp.broadcast_to(new, (tok, hd))
                lrow[idx] = jnp.broadcast_to(total, (tok, hd))

    def attend_if(back):
        pl.when(s >= back)(functools.partial(attend, back))

    depth = (half + 1) // 2
    column, row = s % 2, s // 2
    top = n // 2 - 1

    def kv_copy(owner, target, send_sem, recv_sem):
        ref = kvb.at[jnp.maximum(owner, 0)]
        return pltpu.make_async_remote_copy(
            src_ref=ref,
            dst_ref=ref,
            send_sem=send_sem,
            recv_sem=recv_sem,
            device_id={"sp": target},
            device_id_type=pl.DeviceIdType.MESH,
        )

    def up(j, owner):
        target = jnp.minimum(s + 2, n - 1)
        return kv_copy(owner, target, up_send.at[j - 1], up_recv.at[j - 1])

    def rung(i, owner):
        return kv_copy(owner, s + 1 - 2 * column, rung_send.at[i], rung_recv.at[i])

    def up_sends(j):
        return (row < top) & (row - (j - 1) >= 0)

    def start_up(j):
        @pl.when(up_sends(j))
        def _():
            up(j, s - 2 * (j - 1)).start()

    def wait_up(j):
        @pl.when(row >= j)
        def _():
            up(j, s - 2 * j).wait_recv()

    def rung_owner(i):
        return s - 2 * i - 2 * column

    def start_rung(i, only):
        @pl.when((column == only) & (rung_owner(i) >= 0))
        def _():
            rung(i, rung_owner(i)).start()

    def wait_rung(i):
        @pl.when(s - 1 - 2 * i >= 0)
        def _():
            rung(i, s - 1 - 2 * i).wait_recv()

    def send_own(way):
        for kind in (GATE, VALUE, DOWN):
            send(kind, way, 1)

    local[0].wait()
    start_up(1)
    start_rung(0, 0)
    for i in (1, 2, 3):
        local[i].wait()

    @pl.when(column == 0)
    def _():
        send_own(1)

    @pl.when(column == 1)
    def _():
        send_own(0)

    near = depth <= 2
    if near:
        attend(0)
    for j in range(1, depth + 1):
        wait_up(j)
        if j < depth:
            start_up(j + 1)
            start_rung(j, 0)
        start_rung(j - 1, 1)
        if j == max(depth - 1, 1):

            @pl.when(column == 0)
            def _():
                send_own(0)

            @pl.when(column == 1)
            def _():
                send_own(1)

        if near:
            attend_if(2 * j)
    for i in range(depth):
        wait_rung(i)
        if near:
            attend_if(2 * i + 1)
    if not near:

        @pl.loop(0, jnp.minimum(s, 2 * depth) + 1)
        def _(back):
            attend(back)

    for h in range(heads):
        head = att[2 * h] / lrow[2 * h] - lam_ref[h] * (att[2 * h + 1] / lrow[2 * h + 1])
        scale = lax.rsqrt(jnp.mean(head * head, axis=1, keepdims=True) + epsilon)
        nrm[t, :, pl.ds(h * hd, hd)] = (head * scale * hg_ref[h : h + 1, :]).astype(jnp.bfloat16)

    def peer_copy(src, dst, send_sem, recv_sem, i):
        return pltpu.make_async_remote_copy(
            src_ref=src,
            dst_ref=dst,
            send_sem=send_sem,
            recv_sem=recv_sem,
            device_id={"tp": (t + i) % ntp},
            device_id_type=pl.DeviceIdType.MESH,
        )

    def nrm_copy(i, slot):
        return peer_copy(nrm.at[slot], nrm.at[slot], nrm_send.at[i], nrm_recv.at[i], i)

    for i in range(1, ntp):
        nrm_copy(i, t).start()

    def pass_on(kind, step):
        for way in range(2):
            arrive(kind, way, step)
            if step < half:
                send(kind, way, step + 1)

    pass_on(GATE, 1)
    local[4].wait()
    local[5].wait()
    for i in range(1, ntp):
        nrm_copy(i, (t - i + ntp) % ntp).wait_recv()

    tile = 256

    @pl.loop(0, width // tile)
    def _(c):
        cols = pl.ds(pl.multiple_of(c * tile, tile), tile)
        acc = jnp.zeros((tok, tile), jnp.float32)
        for j in range(ntp):
            acc = acc + jnp.dot(
                nrm[j], owb[pl.ds(j * hw, hw), cols], preferred_element_type=jnp.float32
            )
        stream[:, cols] = acc

    pass_on(VALUE, 1)

    def rms(x, gain):
        return x * lax.rsqrt(jnp.mean(x * x, axis=1, keepdims=True) + epsilon) * gain

    chunk = 16

    @pl.loop(0, tok // chunk)
    def _(c):
        part_rows = pl.ds(pl.multiple_of(c * chunk, chunk), chunk)
        st = resb[part_rows].astype(jnp.float32) + rms(stream[part_rows], mixg_ref[...])
        stream[part_rows] = st
        xn[part_rows] = rms(st, preg_ref[...]).astype(jnp.bfloat16)

    fine = rows % 128 == 0

    def add_block(kind, owner, first):
        acc, w = (gacc, gb) if kind == GATE else (vacc, vb)
        at_rows = pl.ds(pl.multiple_of(owner * rows, rows), rows)
        got = jnp.dot(xn[:, at_rows], w[at_rows, :], preferred_element_type=jnp.float32)
        if first:
            acc[...] = got
        else:
            acc[...] += got

    if fine:
        for kind in (GATE, VALUE):
            add_block(kind, s, True)
    for step in range(1, half + 1):
        for kind in (GATE, VALUE):
            if step > 1:
                pass_on(kind, step)
            if step == half and kind == VALUE:
                pass_on(DOWN, 1)
            if fine:
                add_block(kind, came(0, step), False)
                if step < half:
                    add_block(kind, came(1, step), False)
    if not fine:
        gacc[...] = jnp.dot(xn[...], gb[...], preferred_element_type=jnp.float32)
        vacc[...] = jnp.dot(xn[...], vb[...], preferred_element_type=jnp.float32)

    for i, (acc, ext) in enumerate(((gacc, gext), (vacc, vext))):
        ext[pl.ds(8, tok), :] = acc[...].astype(jnp.bfloat16).astype(jnp.float32)
        halo_out[i] = acc[pl.ds(tok - 16, 16), :].astype(jnp.bfloat16)
        ext[pl.ds(0, 8), :] = jnp.zeros((8, ff), jnp.float32)

    def halo(target):
        return pltpu.make_async_remote_copy(
            src_ref=halo_out,
            dst_ref=halo_in,
            send_sem=halo_send,
            recv_sem=halo_recv,
            device_id={"sp": target},
            device_id_type=pl.DeviceIdType.MESH,
        )

    @pl.when(s < n - 1)
    def _():
        halo(s + 1).start()

    @pl.when(s > 0)
    def _():
        halo(s - 1).wait_recv()
        for i, ext in enumerate((gext, vext)):
            ext[pl.ds(0, 8), :] = halo_in[i].astype(jnp.float32)[8:16]

    before = jnp.maximum(s - 1, 0)
    prev_docs = kvb[before, pl.ds(tok, 16), pl.ds(0, tok)].astype(jnp.float32)[0:1]
    lane_row = lax.broadcasted_iota(jnp.int32, (1, tok), 1)
    last1 = jnp.sum(jnp.where(lane_row == tok - 1, prev_docs, 0.0), axis=1, keepdims=True)
    last2 = jnp.sum(jnp.where(lane_row == tok - 2, prev_docs, 0.0), axis=1, keepdims=True)
    has_prev = s > 0
    last1 = jnp.where(has_prev, last1, -1.0)
    last2 = jnp.where(has_prev, last2, -1.0)
    rowid = lax.broadcasted_iota(jnp.int32, (tok, 1), 0)
    doc1 = jnp.where(rowid == 0, last1, dcol_ref[:, 1:2])
    doc2 = jnp.where(rowid == 0, last2, jnp.where(rowid == 1, last1, dcol_ref[:, 2:3]))
    same1 = doc1 == doc_query
    same2 = doc2 == doc_query

    @pl.loop(0, ff // 128)
    def _(c):
        cols = pl.ds(pl.multiple_of(c * 128, 128), 128)

        def conv(ext, taps):
            w = taps[:, cols]
            total = jnp.where(same2, w[0:1] * ext[pl.ds(6, tok), cols], 0.0)
            total = total + jnp.where(same1, w[1:2] * ext[pl.ds(7, tok), cols], 0.0)
            return total + w[2:3] * ext[pl.ds(8, tok), cols]

        hidden[:, cols] = (
            jax.nn.gelu(conv(gext, gt_ref), approximate=True) * conv(vext, vt_ref)
        ).astype(jnp.bfloat16)

    def rs_copy(i, b, cols):
        peer = (t + i) % ntp
        return peer_copy(
            part.at[pl.ds(pl.multiple_of(peer * share, share), share), cols],
            rsb.at[i - 1, :, cols],
            rs_send.at[b, i],
            rs_recv.at[b, i],
            i,
        )

    def block_cols(owner):
        return pl.ds(pl.multiple_of(owner * rows, rows), rows)

    def down_block(owner, b):
        cols = block_cols(owner)
        part[:, cols] = lax.dot_general(
            hidden[...], db[cols, :], (((1,), (1,)), ((), ())), preferred_element_type=jnp.float32
        ).astype(jnp.bfloat16)
        for i in range(1, ntp):
            rs_copy(i, b, cols).start()

    order = [s]
    if fine:
        down_block(s, 0)
    for step in range(1, half + 1):
        for way in range(2):
            if step > 1:
                arrive(DOWN, way, step)
                if step < half:
                    send(DOWN, way, step + 1)
        for way in range(2 if step < half else 1):
            if fine:
                down_block(came(way, step), len(order))
                order.append(came(way, step))
    if fine:
        pieces = [(b, block_cols(o)) for b, o in enumerate(order)]
    else:

        @pl.loop(0, width // tile)
        def _(c):
            cols = pl.ds(pl.multiple_of(c * tile, tile), tile)
            part[:, cols] = lax.dot_general(
                hidden[...],
                db[cols, :],
                (((1,), (1,)), ((), ())),
                preferred_element_type=jnp.float32,
            ).astype(jnp.bfloat16)

        pieces = [(0, pl.ds(0, width))]
        for i in range(1, ntp):
            rs_copy(i, 0, pieces[0][1]).start()
    for b, cols in pieces:
        for i in range(1, ntp):
            rs_copy(i, b, cols).wait_recv()

    mine = pl.multiple_of(t * share, share)

    pair = ntp == 4
    sibling = jnp.where(t % 2 == 0, 1, ntp - 1)
    turns = [ntp // 2, sibling] if pair else list(range(1, ntp))
    lumps = share // chunk

    def ag_copy(turn, sem, owner, c):
        ref = out_ref.at[pl.ds(pl.multiple_of(owner * share + c * chunk, chunk), chunk)]
        return peer_copy(ref, ref, ag_send.at[sem, c], ag_recv.at[sem, c], turn)

    for c in range(lumps):
        at_rows = pl.ds(pl.multiple_of(mine + c * chunk, chunk), chunk)
        in_rows = pl.ds(c * chunk, chunk)
        lifted = part[at_rows].astype(jnp.float32)
        for i in range(1, ntp):
            lifted = lifted + rsb[i - 1, in_rows].astype(jnp.float32)
        out_ref[at_rows] = (stream[at_rows] + rms(lifted, mlpg_ref[...])).astype(jnp.bfloat16)
        for sem, turn in enumerate(turns):
            ag_copy(turn, sem, t, c).start()
    opposite = (t + ntp // 2) % ntp
    beside = (t + sibling) % ntp
    if pair:
        for c in range(lumps):
            ag_copy(turns[0], 0, opposite, c).wait_recv()
            ag_copy(sibling, 2, opposite, c).start()
        for c in range(lumps):
            ag_copy(sibling, 1, beside, c).wait_recv()
            ag_copy(sibling, 2, (beside + ntp // 2) % ntp, c).wait_recv()
    else:
        for c in range(lumps):
            for sem, turn in enumerate(turns):
                ag_copy(turn, sem, (t - turn + ntp) % ntp, c).wait_recv()

    for kind in (GATE, VALUE, DOWN):
        for way in range(2):
            for step in range(1, half + 1):
                hop(kind, way, step, came(way, step - 1)).wait_send()
    for i in range(1, ntp):
        nrm_copy(i, t).wait_send()
        for b, cols in pieces:
            rs_copy(i, b, cols).wait_send()
    for c in range(lumps):
        for sem, turn in enumerate(turns):
            ag_copy(turn, sem, t, c).wait_send()
        if pair:
            ag_copy(sibling, 2, opposite, c).wait_send()
    for j in range(1, depth + 1):

        @pl.when(up_sends(j))
        def _():
            up(j, s - 2 * (j - 1)).wait_send()

        @pl.when(rung_owner(j - 1) >= 0)
        def _():
            rung(j - 1, rung_owner(j - 1)).wait_send()

    @pl.when(s < n - 1)
    def _():
        halo(s + 1).wait_send()


def per_device(
    n,
    ntp,
    residual,
    queries,
    keys,
    values,
    documents,
    lambdas,
    head_gain,
    out_weight,
    mix_gain,
    pre_gain,
    gate_weight,
    value_weight,
    gate_taps,
    value_taps,
    down_weight,
    mlp_gain,
):
    tok, width = residual.shape
    heads, hd = head_gain.shape
    hw = heads * hd
    rows, ff = gate_weight.shape
    half = n // 2
    share = tok // ntp
    docs = documents.astype(jnp.float32)
    packed = jnp.concatenate([keys.reshape(tok, hw), values.reshape(tok, hw)], axis=1)
    doc_rows = jnp.broadcast_to(
        jnp.pad(docs, (0, 2 * hw - tok)).astype(jnp.bfloat16)[None, :], (EXTRA, 2 * hw)
    )
    kv = jnp.concatenate([packed, doc_rows], axis=0)
    back = [jnp.concatenate([jnp.full((j,), -1.0, jnp.float32), docs[: tok - j]]) for j in (1, 2)]
    dcol = jnp.pad(jnp.stack([docs] + back, axis=1), ((0, 0), (0, 125)))
    score_scale = (hd // 2) ** (-0.5)
    q = (queries.astype(jnp.float32) * score_scale).astype(jnp.bfloat16).reshape(tok, hw)
    bf, f32 = jnp.bfloat16, jnp.float32
    vm = pl.BlockSpec(memory_space=pltpu.VMEM)
    hbm = pl.BlockSpec(memory_space=pl.ANY)
    smem = pl.BlockSpec(memory_space=pltpu.SMEM)
    dma = pltpu.SemaphoreType.DMA
    return pl.pallas_call(
        functools.partial(kernel, n, ntp),
        out_shape=jax.ShapeDtypeStruct((tok, width), bf),
        in_specs=[smem] + [hbm] * 6 + [vm] * 8,
        out_specs=vm,
        scratch_shapes=[
            pltpu.VMEM((n, tok + EXTRA, 2 * hw), bf),
            pltpu.VMEM((n * rows, ff), bf),
            pltpu.VMEM((n * rows, ff), bf),
            pltpu.VMEM((n * rows, ff), bf),
            pltpu.VMEM(out_weight.shape, bf),
            pltpu.VMEM((tok, width), bf),
            pltpu.VMEM((ntp, tok, hw), bf),
            pltpu.VMEM((tok, width), f32),
            pltpu.VMEM((tok, width), bf),
            pltpu.VMEM((tok, ff), f32),
            pltpu.VMEM((tok, ff), f32),
            pltpu.VMEM((tok + 8, ff), f32),
            pltpu.VMEM((tok + 8, ff), f32),
            pltpu.VMEM((2, 16, ff), bf),
            pltpu.VMEM((2, 16, ff), bf),
            pltpu.VMEM((tok, ff), bf),
            pltpu.VMEM((tok, width), bf),
            pltpu.VMEM((ntp - 1, share, width), bf),
            pltpu.VMEM((2 * heads, tok, hd), f32),
            pltpu.VMEM((2 * heads, tok, hd), f32),
            pltpu.VMEM((2 * heads, tok, hd), f32),
            dma((6,)),
            dma((3, 2, half)),
            dma((3, 2, half)),
            dma((half,)),
            dma((half,)),
            dma((half,)),
            dma((half,)),
            dma((ntp,)),
            dma((ntp,)),
            dma,
            dma,
            dma((n, ntp)),
            dma((n, ntp)),
            dma((ntp, share // 16)),
            dma((ntp, share // 16)),
        ],
        compiler_params=pltpu.CompilerParams(
            has_side_effects=True, vmem_limit_bytes=60 * 1024 * 1024
        ),
    )(
        lambdas,
        kv,
        gate_weight,
        value_weight,
        down_weight,
        out_weight,
        residual,
        q,
        dcol,
        head_gain,
        mix_gain[None],
        pre_gain[None],
        gate_taps,
        value_taps,
        mlp_gain[None],
    )


def solution(mesh):
    placed = (
        P("sp", None),
        P("sp", "tp", None),
        P("sp", "tp", None),
        P("sp", "tp", None),
        P("sp"),
        P("tp"),
        P("tp", None),
        P(),
        P(),
        P(),
        P("sp", "tp"),
        P("sp", "tp"),
        P(None, "tp"),
        P(None, "tp"),
        P("sp", "tp"),
        P(),
    )
    body = functools.partial(per_device, mesh.shape["sp"], mesh.shape["tp"])
    return jax.shard_map(
        body, mesh=mesh, in_specs=placed, out_specs=P("sp", None), check_vma=False
    )
```

```python
import functools

import jax
import jax.numpy as jnp
from jax import lax
from jax.experimental import pallas as pl
from jax.experimental.pallas import tpu as pltpu
from jax.sharding import PartitionSpec as P

epsilon = 1e-06
masked_score = -1e30
EXTRA = 16
GATE, VALUE, DOWN, DOWN2 = range(4)


def kernel(
    n,
    ntp,
    lam_ref,
    k_ref,
    v_ref,
    g_hbm,
    v_hbm,
    d_hbm,
    ow_hbm,
    res_hbm,
    q_ref,
    doc_ref,
    hg_ref,
    mixg_ref,
    preg_ref,
    gt_ref,
    vt_ref,
    mlpg_ref,
    out_ref,
    qs,
    kvb,
    gb,
    vb,
    db,
    owb,
    resb,
    nrm,
    stream,
    xn,
    gacc,
    vacc,
    gext,
    vext,
    halo_out,
    halo_in,
    hidden,
    part,
    rsb,
    mrow,
    lrow,
    att,
    local_sem,
    ring_send,
    ring_recv,
    up_send,
    up_recv,
    rung_send,
    rung_recv,
    nrm_send,
    nrm_recv,
    halo_send,
    halo_recv,
    rs_send,
    rs_recv,
    ag_send,
    ag_recv,
):
    s = lax.axis_index("sp")
    t = lax.axis_index("tp")
    half = n // 2
    tok = resb.shape[0]
    width = resb.shape[1]
    rows = g_hbm.shape[0]
    ff = g_hbm.shape[1]
    heads = hg_ref.shape[0]
    hd = hg_ref.shape[1]
    hw = heads * hd
    share = tok // ntp
    pos = jnp.where(s % 2 == 0, s // 2, n - 1 - s // 2)

    def at(p):
        p = (p + n) % n
        return jnp.where(p < half, 2 * p, 2 * n - 1 - 2 * p)

    neighbour = (at(pos + 1), at(pos - 1))

    def place(kind, owner, piece):
        ref = (gb, vb, db, db)[kind]
        if piece is None:
            return ref.at[pl.ds(pl.multiple_of(owner * rows, rows), rows)]
        return ref.at[pl.ds(pl.multiple_of(owner * rows + piece * (rows // 2), rows // 2), rows // 2)]

    def hop(kind, way, step, owner):
        piece = way if step == half else None
        if kind >= DOWN:
            piece = kind - DOWN
        ref = place(kind, owner, piece)
        return pltpu.make_async_remote_copy(
            src_ref=ref,
            dst_ref=ref,
            send_sem=ring_send.at[kind, way, step - 1],
            recv_sem=ring_recv.at[kind, way, step - 1],
            device_id={"sp": neighbour[way]},
            device_id_type=pl.DeviceIdType.MESH,
        )

    def came(way, step):
        return at(pos - step) if way == 0 else at(pos + step)

    def used(kind, way, step):
        return kind < DOWN or step < half or kind - DOWN == way

    def send(kind, way, step):
        if used(kind, way, step):
            hop(kind, way, step, came(way, step - 1)).start()

    def arrive(kind, way, step):
        if used(kind, way, step):
            hop(kind, way, step, came(way, step)).wait_recv()

    local = [
        pltpu.make_async_copy(src, dst, local_sem.at[i])
        for i, (src, dst) in enumerate(
            (
                (g_hbm, place(GATE, s, None)),
                (v_hbm, place(VALUE, s, None)),
                (d_hbm, place(DOWN, s, None)),
                (ow_hbm, owb),
                (res_hbm, resb),
            )
        )
    ]
    for copy in local:
        copy.start()
    mrow[...] = jnp.full(mrow.shape, masked_score, jnp.float32)
    lrow[...] = jnp.zeros(lrow.shape, jnp.float32)
    att[...] = jnp.zeros(att.shape, jnp.float32)
    on_row = lax.broadcasted_iota(jnp.int32, (tok, tok), 0)
    on_lane = lax.broadcasted_iota(jnp.int32, (tok, tok), 1)

    def doc_before(shift):
        spread = jnp.broadcast_to(doc_ref[...].astype(jnp.float32), (tok, tok))
        return jnp.sum(jnp.where(on_row - shift == on_lane, spread, 0.0), axis=1, keepdims=True)

    doc_query = doc_before(0)
    lane = lax.broadcasted_iota(jnp.int32, (tok, hd), 1)
    delta = lax.broadcasted_iota(jnp.int32, (tok, tok), 0) - lax.broadcasted_iota(
        jnp.int32, (tok, tok), 1
    )

    def attend(back):
        o = s - back
        doc_key = kvb[o, pl.ds(tok, 16), pl.ds(0, tok)].astype(jnp.float32)[0:1]
        allowed = (delta + back * tok >= 0) & (doc_key == doc_query)
        for h in range(heads):
            k = kvb[o, pl.ds(0, tok), pl.ds(h * hd, hd)]
            val = kvb[o, pl.ds(0, tok), pl.ds(hw + h * hd, hd)]
            qh = qs[:, h * hd : (h + 1) * hd]
            for m in range(2):
                keep = lane < hd // 2 if m == 0 else lane >= hd // 2
                qm = jnp.where(keep, qh, jnp.zeros_like(qh))
                scores = lax.dot_general(
                    qm, k, (((1,), (1,)), ((), ())), preferred_element_type=jnp.float32
                )
                scores = jnp.where(allowed, scores, masked_score)
                idx = h * 2 + m
                old = mrow[idx, :, 0:1]
                new = jnp.maximum(old, jnp.max(scores, axis=1, keepdims=True))
                probs = jnp.exp(scores - new)
                factor = jnp.exp(old - new)
                total = lrow[idx, :, 0:1] * factor + jnp.sum(probs, axis=1, keepdims=True)
                att[idx] = att[idx] * factor + jnp.dot(
                    probs.astype(jnp.bfloat16), val, preferred_element_type=jnp.float32
                )
                mrow[idx] = jnp.broadcast_to(new, (tok, hd))
                lrow[idx] = jnp.broadcast_to(total, (tok, hd))

    def attend_if(back):
        pl.when(s >= back)(functools.partial(attend, back))

    depth = (half + 1) // 2
    column, row = s % 2, s // 2
    top = n // 2 - 1

    def kv_copy(owner, target, send_sem, recv_sem):
        ref = kvb.at[jnp.maximum(owner, 0)]
        return pltpu.make_async_remote_copy(
            src_ref=ref,
            dst_ref=ref,
            send_sem=send_sem,
            recv_sem=recv_sem,
            device_id={"sp": target},
            device_id_type=pl.DeviceIdType.MESH,
        )

    def up(j, owner):
        target = jnp.minimum(s + 2, n - 1)
        return kv_copy(owner, target, up_send.at[j - 1], up_recv.at[j - 1])

    def rung(i, owner):
        return kv_copy(owner, s + 1 - 2 * column, rung_send.at[i], rung_recv.at[i])

    def up_sends(j):
        return (row < top) & (row - (j - 1) >= 0)

    def start_up(j):
        @pl.when(up_sends(j))
        def _():
            up(j, s - 2 * (j - 1)).start()

    def wait_up(j):
        @pl.when(row >= j)
        def _():
            up(j, s - 2 * j).wait_recv()

    def rung_owner(i):
        return s - 2 * i - 2 * column

    def start_rung(i, only):
        @pl.when((column == only) & (rung_owner(i) >= 0))
        def _():
            rung(i, rung_owner(i)).start()

    def wait_rung(i):
        @pl.when(s - 1 - 2 * i >= 0)
        def _():
            rung(i, s - 1 - 2 * i).wait_recv()

    def send_own(free_way, kinds):
        for c in range(2):

            @pl.when(column == c)
            def _():
                for kind in kinds:
                    send(kind, free_way if c == 0 else 1 - free_way, 1)

    for i in (0, 1, 2):
        local[i].wait()
    send_own(1, (GATE, VALUE, DOWN, DOWN2))
    doc_row = doc_ref[...].astype(jnp.float32)
    kvb[s, pl.ds(tok, 16), pl.ds(0, tok)] = jnp.broadcast_to(doc_row, (16, tok)).astype(
        jnp.bfloat16
    )
    for h in range(heads):
        kvb[s, pl.ds(0, tok), pl.ds(h * hd, hd)] = k_ref[:, h, :]
        kvb[s, pl.ds(0, tok), pl.ds(hw + h * hd, hd)] = v_ref[:, h, :]
    for h in range(heads):
        qs[:, h * hd : (h + 1) * hd] = (
            q_ref[:, h, :].astype(jnp.float32) * (hd // 2) ** (-0.5)
        ).astype(jnp.bfloat16)
    start_up(1)
    start_rung(0, 0)
    send_own(0, (GATE,))

    near = depth <= 2
    if near:
        attend(0)
    for j in range(1, depth + 1):
        wait_up(j)
        if j < depth:
            start_up(j + 1)
            start_rung(j, 0)
        start_rung(j - 1, 1)
        if j == max(depth - 1, 1):
            send_own(0, (VALUE, DOWN, DOWN2))
        if near:
            attend_if(2 * j)
    for i in range(depth):
        wait_rung(i)
        if near:
            attend_if(2 * i + 1)
    if not near:

        @pl.loop(0, jnp.minimum(s, 2 * depth) + 1)
        def _(back):
            attend(back)

    for h in range(heads):
        head = att[2 * h] / lrow[2 * h] - lam_ref[h] * (att[2 * h + 1] / lrow[2 * h + 1])
        scale = lax.rsqrt(jnp.mean(head * head, axis=1, keepdims=True) + epsilon)
        nrm[t, :, pl.ds(h * hd, hd)] = (head * scale * hg_ref[h : h + 1, :]).astype(jnp.bfloat16)

    def peer_copy(src, dst, send_sem, recv_sem, i):
        return pltpu.make_async_remote_copy(
            src_ref=src,
            dst_ref=dst,
            send_sem=send_sem,
            recv_sem=recv_sem,
            device_id={"tp": (t + i) % ntp},
            device_id_type=pl.DeviceIdType.MESH,
        )

    def nrm_copy(i, slot):
        return peer_copy(nrm.at[slot], nrm.at[slot], nrm_send.at[i], nrm_recv.at[i], i)

    for i in range(1, ntp):
        nrm_copy(i, t).start()

    def pass_on(kind, step):
        for way in range(2):
            arrive(kind, way, step)
            if step < half:
                send(kind, way, step + 1)

    pass_on(GATE, 1)
    local[3].wait()
    local[4].wait()
    for i in range(1, ntp):
        nrm_copy(i, (t - i + ntp) % ntp).wait_recv()

    tile = 256

    @pl.loop(0, width // tile)
    def _(c):
        cols = pl.ds(pl.multiple_of(c * tile, tile), tile)
        acc = jnp.zeros((tok, tile), jnp.float32)
        for j in range(ntp):
            acc = acc + jnp.dot(
                nrm[j], owb[pl.ds(j * hw, hw), cols], preferred_element_type=jnp.float32
            )
        stream[:, cols] = acc

    pass_on(VALUE, 1)

    def rms(x, gain):
        return x * lax.rsqrt(jnp.mean(x * x, axis=1, keepdims=True) + epsilon) * gain

    chunk = 16

    @pl.loop(0, tok // chunk)
    def _(c):
        part_rows = pl.ds(pl.multiple_of(c * chunk, chunk), chunk)
        st = resb[part_rows].astype(jnp.float32) + rms(stream[part_rows], mixg_ref[...])
        stream[part_rows] = st
        xn[part_rows] = rms(st, preg_ref[...]).astype(jnp.bfloat16)

    fine = rows % 128 == 0

    def add_block(kind, owner, first):
        acc, w = (gacc, gb) if kind == GATE else (vacc, vb)
        at_rows = pl.ds(pl.multiple_of(owner * rows, rows), rows)
        got = jnp.dot(xn[:, at_rows], w[at_rows, :], preferred_element_type=jnp.float32)
        if first:
            acc[...] = got
        else:
            acc[...] += got

    if fine:
        for kind in (GATE, VALUE):
            add_block(kind, s, True)
    for step in range(1, half + 1):
        for kind in (GATE, VALUE):
            if step > 1:
                pass_on(kind, step)
            if step == half and kind == VALUE:
                pass_on(DOWN, 1)
                pass_on(DOWN2, 1)
            if fine:
                add_block(kind, came(0, step), False)
                if step < half:
                    add_block(kind, came(1, step), False)
    if not fine:
        gacc[...] = jnp.dot(xn[...], gb[...], preferred_element_type=jnp.float32)
        vacc[...] = jnp.dot(xn[...], vb[...], preferred_element_type=jnp.float32)

    for i, (acc, ext) in enumerate(((gacc, gext), (vacc, vext))):
        ext[pl.ds(8, tok), :] = acc[...].astype(jnp.bfloat16).astype(jnp.float32)
        halo_out[i] = acc[pl.ds(tok - 16, 16), :].astype(jnp.bfloat16)
        ext[pl.ds(0, 8), :] = jnp.zeros((8, ff), jnp.float32)

    def halo(target):
        return pltpu.make_async_remote_copy(
            src_ref=halo_out,
            dst_ref=halo_in,
            send_sem=halo_send,
            recv_sem=halo_recv,
            device_id={"sp": target},
            device_id_type=pl.DeviceIdType.MESH,
        )

    @pl.when(s < n - 1)
    def _():
        halo(s + 1).start()

    @pl.when(s > 0)
    def _():
        halo(s - 1).wait_recv()
        for i, ext in enumerate((gext, vext)):
            ext[pl.ds(0, 8), :] = halo_in[i].astype(jnp.float32)[8:16]

    before = jnp.maximum(s - 1, 0)
    prev_docs = kvb[before, pl.ds(tok, 16), pl.ds(0, tok)].astype(jnp.float32)[0:1]
    lane_row = lax.broadcasted_iota(jnp.int32, (1, tok), 1)
    last1 = jnp.sum(jnp.where(lane_row == tok - 1, prev_docs, 0.0), axis=1, keepdims=True)
    last2 = jnp.sum(jnp.where(lane_row == tok - 2, prev_docs, 0.0), axis=1, keepdims=True)
    has_prev = s > 0
    last1 = jnp.where(has_prev, last1, -1.0)
    last2 = jnp.where(has_prev, last2, -1.0)
    rowid = lax.broadcasted_iota(jnp.int32, (tok, 1), 0)
    doc1 = jnp.where(rowid == 0, last1, doc_before(1))
    doc2 = jnp.where(rowid == 0, last2, jnp.where(rowid == 1, last1, doc_before(2)))
    same1 = doc1 == doc_query
    same2 = doc2 == doc_query

    @pl.loop(0, ff // 128)
    def _(c):
        cols = pl.ds(pl.multiple_of(c * 128, 128), 128)

        def conv(ext, taps):
            w = taps[:, cols]
            total = jnp.where(same2, w[0:1] * ext[pl.ds(6, tok), cols], 0.0)
            total = total + jnp.where(same1, w[1:2] * ext[pl.ds(7, tok), cols], 0.0)
            return total + w[2:3] * ext[pl.ds(8, tok), cols]

        hidden[:, cols] = (
            jax.nn.gelu(conv(gext, gt_ref), approximate=True) * conv(vext, vt_ref)
        ).astype(jnp.bfloat16)

    def rs_copy(i, b, cols):
        peer = (t + i) % ntp
        return peer_copy(
            part.at[pl.ds(pl.multiple_of(peer * share, share), share), cols],
            rsb.at[i - 1, :, cols],
            rs_send.at[b, i],
            rs_recv.at[b, i],
            i,
        )

    def block_cols(owner):
        return pl.ds(pl.multiple_of(owner * rows, rows), rows)

    def down_block(owner, b):
        cols = block_cols(owner)
        part[:, cols] = lax.dot_general(
            hidden[...], db[cols, :], (((1,), (1,)), ((), ())), preferred_element_type=jnp.float32
        ).astype(jnp.bfloat16)
        for i in range(1, ntp):
            rs_copy(i, b, cols).start()

    order = [s]
    if fine:
        down_block(s, 0)
    for step in range(1, half + 1):
        if step > 1:
            pass_on(DOWN, step)
            pass_on(DOWN2, step)
        for way in range(2 if step < half else 1):
            if fine:
                down_block(came(way, step), len(order))
                order.append(came(way, step))
    if fine:
        pieces = [(b, block_cols(o)) for b, o in enumerate(order)]
    else:

        @pl.loop(0, width // tile)
        def _(c):
            cols = pl.ds(pl.multiple_of(c * tile, tile), tile)
            part[:, cols] = lax.dot_general(
                hidden[...],
                db[cols, :],
                (((1,), (1,)), ((), ())),
                preferred_element_type=jnp.float32,
            ).astype(jnp.bfloat16)

        pieces = [(0, pl.ds(0, width))]
        for i in range(1, ntp):
            rs_copy(i, 0, pieces[0][1]).start()
    for b, cols in pieces:
        for i in range(1, ntp):
            rs_copy(i, b, cols).wait_recv()

    mine = pl.multiple_of(t * share, share)

    pair = ntp == 4
    sibling = jnp.where(t % 2 == 0, 1, ntp - 1)
    turns = [ntp // 2, sibling] if pair else list(range(1, ntp))
    lumps = share // chunk

    def ag_copy(turn, sem, owner, c):
        ref = out_ref.at[pl.ds(pl.multiple_of(owner * share + c * chunk, chunk), chunk)]
        return peer_copy(ref, ref, ag_send.at[sem, c], ag_recv.at[sem, c], turn)

    for c in range(lumps):
        at_rows = pl.ds(pl.multiple_of(mine + c * chunk, chunk), chunk)
        in_rows = pl.ds(c * chunk, chunk)
        lifted = part[at_rows].astype(jnp.float32)
        for i in range(1, ntp):
            lifted = lifted + rsb[i - 1, in_rows].astype(jnp.float32)
        out_ref[at_rows] = (stream[at_rows] + rms(lifted, mlpg_ref[...])).astype(jnp.bfloat16)
        for sem, turn in enumerate(turns):
            ag_copy(turn, sem, t, c).start()
    opposite = (t + ntp // 2) % ntp
    beside = (t + sibling) % ntp
    if pair:
        for c in range(lumps):
            ag_copy(turns[0], 0, opposite, c).wait_recv()
            ag_copy(sibling, 2, opposite, c).start()
        for c in range(lumps):
            ag_copy(sibling, 1, beside, c).wait_recv()
            ag_copy(sibling, 2, (beside + ntp // 2) % ntp, c).wait_recv()
    else:
        for c in range(lumps):
            for sem, turn in enumerate(turns):
                ag_copy(turn, sem, (t - turn + ntp) % ntp, c).wait_recv()

    for kind in range(4):
        for way in range(2):
            for step in range(1, half + 1):
                if used(kind, way, step):
                    hop(kind, way, step, came(way, step - 1)).wait_send()
    for i in range(1, ntp):
        nrm_copy(i, t).wait_send()
        for b, cols in pieces:
            rs_copy(i, b, cols).wait_send()
    for c in range(lumps):
        for sem, turn in enumerate(turns):
            ag_copy(turn, sem, t, c).wait_send()
        if pair:
            ag_copy(sibling, 2, opposite, c).wait_send()
    for j in range(1, depth + 1):

        @pl.when(up_sends(j))
        def _():
            up(j, s - 2 * (j - 1)).wait_send()

        @pl.when(rung_owner(j - 1) >= 0)
        def _():
            rung(j - 1, rung_owner(j - 1)).wait_send()

    @pl.when(s < n - 1)
    def _():
        halo(s + 1).wait_send()


def per_device(
    n,
    ntp,
    residual,
    queries,
    keys,
    values,
    documents,
    lambdas,
    head_gain,
    out_weight,
    mix_gain,
    pre_gain,
    gate_weight,
    value_weight,
    gate_taps,
    value_taps,
    down_weight,
    mlp_gain,
):
    tok, width = residual.shape
    heads, hd = head_gain.shape
    hw = heads * hd
    rows, ff = gate_weight.shape
    half = n // 2
    share = tok // ntp
    bf, f32 = jnp.bfloat16, jnp.float32
    vm = pl.BlockSpec(memory_space=pltpu.VMEM)
    hbm = pl.BlockSpec(memory_space=pl.ANY)
    smem = pl.BlockSpec(memory_space=pltpu.SMEM)
    dma = pltpu.SemaphoreType.DMA
    return pl.pallas_call(
        functools.partial(kernel, n, ntp),
        out_shape=jax.ShapeDtypeStruct((tok, width), bf),
        in_specs=[smem] + [vm] * 2 + [hbm] * 5 + [vm] * 8,
        out_specs=vm,
        scratch_shapes=[
            pltpu.VMEM((tok, hw), bf),
            pltpu.VMEM((n, tok + EXTRA, 2 * hw), bf),
            pltpu.VMEM((n * rows, ff), bf),
            pltpu.VMEM((n * rows, ff), bf),
            pltpu.VMEM((n * rows, ff), bf),
            pltpu.VMEM(out_weight.shape, bf),
            pltpu.VMEM((tok, width), bf),
            pltpu.VMEM((ntp, tok, hw), bf),
            pltpu.VMEM((tok, width), f32),
            pltpu.VMEM((tok, width), bf),
            pltpu.VMEM((tok, ff), f32),
            pltpu.VMEM((tok, ff), f32),
            pltpu.VMEM((tok + 8, ff), f32),
            pltpu.VMEM((tok + 8, ff), f32),
            pltpu.VMEM((2, 16, ff), bf),
            pltpu.VMEM((2, 16, ff), bf),
            pltpu.VMEM((tok, ff), bf),
            pltpu.VMEM((tok, width), bf),
            pltpu.VMEM((ntp - 1, share, width), bf),
            pltpu.VMEM((2 * heads, tok, hd), f32),
            pltpu.VMEM((2 * heads, tok, hd), f32),
            pltpu.VMEM((2 * heads, tok, hd), f32),
            dma((6,)),
            dma((4, 2, half)),
            dma((4, 2, half)),
            dma((half,)),
            dma((half,)),
            dma((half,)),
            dma((half,)),
            dma((ntp,)),
            dma((ntp,)),
            dma,
            dma,
            dma((n, ntp)),
            dma((n, ntp)),
            dma((ntp, share // 16)),
            dma((ntp, share // 16)),
        ],
        compiler_params=pltpu.CompilerParams(
            has_side_effects=True, vmem_limit_bytes=60 * 1024 * 1024
        ),
    )(
        lambdas,
        keys,
        values,
        gate_weight,
        value_weight,
        down_weight,
        out_weight,
        residual,
        queries,
        documents[None],
        head_gain,
        mix_gain[None],
        pre_gain[None],
        gate_taps,
        value_taps,
        mlp_gain[None],
    )


def solution(mesh):
    placed = (
        P("sp", None),
        P("sp", "tp", None),
        P("sp", "tp", None),
        P("sp", "tp", None),
        P("sp"),
        P("tp"),
        P("tp", None),
        P(),
        P(),
        P(),
        P("sp", "tp"),
        P("sp", "tp"),
        P(None, "tp"),
        P(None, "tp"),
        P("sp", "tp"),
        P(),
    )
    body = functools.partial(per_device, mesh.shape["sp"], mesh.shape["tp"])
    return jax.shard_map(
        body, mesh=mesh, in_specs=placed, out_specs=P("sp", None), check_vma=False
    )
```
